32 devices in a mesh: sp: 4 (over y, x), tp: 8 (over z, core).
Axes of the slice: x: 2, y: 2, z: 4, core: 2. Of those that a mesh axis runs over, the one named last changes fastest.
Arguments:
- saved_input: bfloat16 [1024, 2048], P('sp'), may hold values from -6 to 6
- cotangent: bfloat16 [1024, 2048], P('sp'), may hold values from -6 to 6
- expert_ids: int32 [1024, 2], P('sp'), may hold values from 0 to 3, all different within a row; in each aligned block of 256 rows (0 to 255, 256 to 511, ...) at most 256 rows name the same one
- route_weight: float32 [1024, 2], P('sp'), may hold values from 0.1 to 0.9
- w_gate: bfloat16 [4, 2048, 6144], P('sp', None, 'tp'), may hold values from -0.125 to 0.125
- w_up: bfloat16 [4, 2048, 6144], P('sp', None, 'tp'), may hold values from -0.125 to 0.125
- w_down: bfloat16 [4, 6144, 2048], P('sp', 'tp'), may hold values from -0.078125 to 0.078125
- w_out: bfloat16 [2048, 2048], P(None, 'tp'), may hold values from -0.125 to 0.125
- channel_gain: float32 [2048], P('tp'), may hold values from 0.1 to 1.9
- conv_taps: float32 [31, 2048], P(None, 'tp'), may hold values from -1 to 1
- glu_value: bfloat16 [2048, 1024], P('tp', 'sp'), may hold values from -6 to 6
- glu_gate: bfloat16 [2048, 1024], P('tp', 'sp'), may hold values from -8 to 8
- conv_out: bfloat16 [2048, 1024], P('tp', 'sp'), may hold values from -6 to 6
- norm_mean: float32 [1024], P('sp'), may hold values from -3 to 3
- norm_rstd: float32 [1024], P('sp'), may hold values from 0.5 to 2
Outputs:
- gate_grad: bfloat16 [4, 2048, 6144], P('sp', None, 'tp')
- up_grad: bfloat16 [4, 2048, 6144], P('sp', None, 'tp')
- down_grad: bfloat16 [4, 6144, 2048], P('sp', 'tp')
- proj_grad: float32 [2048, 2048], P('sp', 'tp')
- value_grad: bfloat16 [2048, 1024], P('tp', 'sp')
- gate_in_grad: bfloat16 [2048, 1024], P('tp', 'sp')
The draws below stay inside these ranges and needn't reach their ends.
Inputs may be any that keep to these rules, and one draw needn't show every extreme that they name: `expert_ids`: the two experts of a position differ. In the positions of one block of 256, no expert is named more than 256 times, a bound that some block reaches.
All inputs are finite; a program needn't handle non-finite values.
Results may differ from the reference program's by a relative error of at most 0.018.
Values may be sent and summed in bfloat16 or wider, within the bound.
A program may use at most 128 MiB of HBM per device.

```python
import math
import jax
import jax.numpy as jnp
import numpy as np
from jax import lax

D = 2048
C = 2048
FF = 6144
CONV_K = 31
TOK_SP = 256
EXPERTS = 4
TOKENS = 1024
CAP = 256
N_SP = 4


def strengthened(drawn, key, source, target, blocks, factor):
    owner, partner = [(jnp.arange(drawn.shape[dim]) // (drawn.shape[dim] // blocks)).reshape([-1 if axis == dim else 1 for axis in range(drawn.ndim)]) for dim in (source, target)]
    chosen = jax.random.permutation(key, blocks)[partner]
    strong = (owner == chosen) | (owner == (partner + blocks // 2) % blocks)
    return jnp.where(strong, factor * drawn, drawn)


def levels(stream_key, dims, split, least, high):
    level = 1.0
    for position, blocks in split:
        heights = jax.random.uniform(jax.random.fold_in(jax.random.fold_in(stream_key, 6), position), (blocks,), jnp.float32, least / len(split), high / len(split))
        level = level * jnp.repeat(jnp.exp(heights), dims[position] // blocks).reshape((-1,) + (1,) * (len(dims) - 1 - position))
    return level


def shared_out(key, own, number, rows, amount, top, bound, skew):
    sequence = jax.random.permutation(key, amount)
    crowded, usual = portions_of(amount, rows * top, bound, skew, True), portions_of(amount, rows * top, bound, skew, False)
    places = jnp.arange(amount)

    def named(tallies, rotation):
        used = int((tallies > 0).sum())
        fixed = max(1, used // 4)
        shifted = fixed + (places - fixed + rotation * (used - fixed)) % max(1, amount - fixed)
        return jnp.zeros((amount,), jnp.int32).at[sequence[jnp.where(places < fixed, places, shifted)]].set(jnp.asarray(tallies, jnp.int32))

    tallies = jnp.where(number % 4 == 0, named(crowded, number // 4), named(usual, number - number // 4 - 1))
    mixed = jax.random.permutation(jax.random.fold_in(own, 3), amount)
    giver, taker = mixed[0:amount // 2 * 2:2], mixed[1:amount // 2 * 2:2]
    room = jnp.minimum(tallies[giver] - 1, bound - tallies[taker]) // 2
    room = jnp.where((giver == sequence[0]) | (taker == sequence[0]) | (tallies[taker] == 0), 0, jnp.maximum(room, 0))
    shifted = jax.random.randint(jax.random.fold_in(own, 4), (amount // 2,), 0, 1 << 20) % (room + 1)
    tallies = tallies.at[giver].add(-shifted).at[taker].add(shifted)
    items = jnp.searchsorted(jnp.cumsum(tallies), jnp.arange(rows * top), side="right").astype(jnp.int32)
    grid = items.reshape(top, rows).T
    grid = grid[jax.random.permutation(jax.random.fold_in(own, 1), rows)]
    rotation = jax.random.randint(jax.random.fold_in(own, 2), (rows, 1), 0, top)
    return jnp.take_along_axis(grid, (jnp.arange(top)[None, :] + rotation) % top, axis=1)


def portions_of(number_of, total, most, lean, full):
    loads = [(1 << 20) // math.isqrt(standing ** lean) + 1 for standing in range(1, number_of + 1)]
    largest = most if full else min(most, max(-(-total // number_of), total * loads[0] // sum(loads)))
    least = 1 if total - largest >= number_of - 1 else 0
    given, rest = [largest] + [least] * (number_of - 1), total - largest - least * (number_of - 1)
    while rest > 0:
        movable = [i for i in range(1, number_of) if given[i] < largest] or [i for i in range(1, number_of) if given[i] < most]
        whole, budget = sum([loads[i] for i in movable]), rest
        for i in movable:
            addition = min(most - given[i], max(1, budget * loads[i] // whole), rest)
            given[i] = given[i] + addition
            rest = rest - addition
    return np.array(given)


def gaussian(stream_key, dims, deviation, reach, pieces=(), held_as=jnp.bfloat16):
    factor_of = levels(stream_key, dims, pieces, -0.22, 0.18) if pieces else 1.0
    result = jax.random.normal(stream_key, dims, jnp.float32) * deviation * factor_of
    return jnp.minimum(jnp.maximum(result, -reach), reach).astype(held_as)


def bell_draw_with(key, extent, scale, reach, shards, heavy, held_as=jnp.bfloat16):
    drawn = scale * jax.random.normal(key, extent, jnp.float32)
    if shards:
        drawn = drawn * levels(key, extent, shards, -0.22, 0.18)
    return jnp.clip(strengthened(drawn, jax.random.fold_in(key, 3), *heavy), -reach, reach).astype(held_as)


def setup_inputs(seed: int = 0) -> dict:
    key_list = jax.random.split(jax.random.key(seed), 16)
    saved_input = gaussian(key_list[0], (TOKENS, D), 1.0, 6.0, ((0, 4),))
    cotangent = bell_draw_with(key_list[1], (TOKENS, D), 1.0, 6.0, ((0, 4),), (0, 1, 4, 2.0))
    expert_ids_keys = jax.random.split(jax.random.fold_in(key_list[2], 1), TOKENS // TOK_SP)
    expert_ids_turns = jax.random.permutation(jax.random.fold_in(key_list[2], 3), TOKENS // TOK_SP)
    expert_ids = jax.vmap(lambda own, number: shared_out(jax.random.fold_in(key_list[2], 2), own, number, TOK_SP, EXPERTS, 2, CAP, 1))(expert_ids_keys, expert_ids_turns).reshape((TOKENS, 2))
    route_weight = jnp.clip(0.1 + 0.79999997 * jax.random.uniform(key_list[3], (TOKENS, 2), jnp.float32) ** levels(key_list[3], (TOKENS, 2), ((0, 4),), -0.2, 0.2), 0.1, 0.9)
    w_gate = gaussian(key_list[4], (EXPERTS, D, FF), D ** -0.5, 0.125, ((0, 4), (2, 8)))
    w_up = gaussian(key_list[5], (EXPERTS, D, FF), D ** -0.5, 0.125, ((0, 4), (2, 8)))
    w_down = gaussian(key_list[6], (EXPERTS, FF, D), FF ** -0.5, 0.078125, ((0, 4), (1, 8)))
    w_out = gaussian(key_list[7], (D, C), C ** -0.5, 0.125, ((1, 8),))
    channel_gain = jnp.clip(1.0 + 0.18 * jax.random.normal(key_list[8], (C,), jnp.float32), 0.1, 1.9)
    conv_taps = gaussian(key_list[9], (CONV_K, C), CONV_K ** -0.5, 1.0, ((1, 8),), jnp.float32)
    glu_value = gaussian(key_list[10], (C, TOKENS), 1.0, 6.0, ((0, 8), (1, 4)))
    glu_gate = gaussian(key_list[11], (C, TOKENS), 1.5, 8.0, ((0, 8), (1, 4)))
    conv_out = gaussian(key_list[12], (C, TOKENS), 1.0, 6.0, ((0, 8), (1, 4)))
    norm_mean = gaussian(key_list[13], (TOKENS,), 0.5, 3.0, ((0, 4),), jnp.float32)
    norm_rstd = jnp.clip(jnp.exp(math.log(2.0) - 1.3862944 * jax.random.uniform(key_list[14], (TOKENS,), jnp.float32) ** levels(key_list[14], (TOKENS,), ((0, 4),), -0.2, 0.2)), 0.5, 2.0)
    return dict(saved_input=saved_input, cotangent=cotangent, expert_ids=expert_ids, route_weight=route_weight, w_gate=w_gate, w_up=w_up, w_down=w_down, w_out=w_out, channel_gain=channel_gain, conv_taps=conv_taps, glu_value=glu_value, glu_gate=glu_gate, conv_out=conv_out, norm_mean=norm_mean, norm_rstd=norm_rstd)


def contract(left, right, left_dim, right_dim):
    return lax.dot_general(left, right, (((left_dim,), (right_dim,)), ((), ())), preferred_element_type=jnp.float32)


def expert_grads(rows_in, rows_cot, gate_weight, up_weight, down_weight):
    gate_pre = jnp.dot(rows_in, gate_weight, preferred_element_type=jnp.float32)
    up_pre = jnp.dot(rows_in, up_weight, preferred_element_type=jnp.float32)
    sigma = jax.nn.sigmoid(gate_pre)
    hidden = (gate_pre * sigma * up_pre).astype(jnp.bfloat16)
    hidden_cot = contract(rows_cot, down_weight, 1, 1)
    down_part = contract(hidden, rows_cot, 0, 0).astype(jnp.bfloat16)
    gate_cot = (hidden_cot * up_pre * sigma * (1.0 + gate_pre * (1.0 - sigma))).astype(jnp.bfloat16)
    up_cot = (hidden_cot * gate_pre * sigma).astype(jnp.bfloat16)
    gate_part = contract(rows_in, gate_cot, 0, 0).astype(jnp.bfloat16)
    up_part = contract(rows_in, up_cot, 0, 0).astype(jnp.bfloat16)
    input_cot = contract(gate_cot, gate_weight, 1, 1) + contract(up_cot, up_weight, 1, 1)
    return gate_part, up_part, down_part, input_cot


def reference(saved_input, cotangent, expert_ids, route_weight, w_gate, w_up, w_down, w_out,
              channel_gain, conv_taps, glu_value, glu_gate, conv_out, norm_mean, norm_rstd):
    pairs = expert_ids.reshape(N_SP, 2 * TOK_SP)
    onehot = (pairs[:, :, None] == jnp.arange(EXPERTS, dtype=jnp.int32)[None, None, :]).astype(jnp.int32)
    before = jnp.cumsum(onehot, axis=1) - onehot
    slots = jnp.sum(before * onehot, axis=2)
    source = jnp.arange(N_SP, dtype=jnp.int32)[:, None]
    target = (pairs * (N_SP * CAP) + source * CAP + slots).reshape(2 * TOKENS).astype(jnp.int32)
    owner = jnp.zeros((EXPERTS * N_SP * CAP,), jnp.int32).at[target].set(jnp.arange(2 * TOKENS, dtype=jnp.int32) + 1)
    filled = (owner > 0)[:, None]
    pair_index = jnp.maximum(owner - 1, 0)
    scaled = (route_weight[:, :, None] * cotangent.astype(jnp.float32)[:, None, :]).astype(jnp.bfloat16)
    scaled = scaled.reshape(2 * TOKENS, D)
    rows_cot = jnp.where(filled, scaled[pair_index], jnp.zeros_like(scaled[:1])).reshape(EXPERTS, N_SP * CAP, D)
    rows_in = jnp.where(filled, saved_input[pair_index // 2], jnp.zeros_like(saved_input[:1]))
    rows_in = rows_in.reshape(EXPERTS, N_SP * CAP, D)
    gate_grad, up_grad, down_grad, input_cot = lax.map(
        lambda packed: expert_grads(*packed), (rows_in, rows_cot, w_gate, w_up, w_down))
    routed = input_cot.reshape(EXPERTS * N_SP * CAP, D)[target].reshape(TOKENS, 2, D)
    mixed_cot = (cotangent.astype(jnp.float32) + jnp.sum(routed, axis=1)).astype(jnp.bfloat16)

    centered = (conv_out.astype(jnp.float32) - norm_mean[None, :]) * norm_rstd[None, :]
    normed = centered * channel_gain[:, None]
    sigma = jax.nn.sigmoid(normed)
    output_act = (normed * sigma).astype(jnp.bfloat16)
    proj_grad = contract(mixed_cot, output_act, 0, 1)
    act_cot = contract(w_out, mixed_cot, 0, 1)
    norm_cot = act_cot * sigma * (1.0 + normed * (1.0 - sigma)) * channel_gain[:, None]
    first_sum = jnp.sum(norm_cot, axis=0)
    second_sum = jnp.sum(norm_cot * centered, axis=0)
    conv_cot = norm_rstd[None, :] * (norm_cot - first_sum[None, :] / C - centered * second_sum[None, :] / C)
    padded = jnp.pad(conv_cot, ((0, 0), (0, CONV_K - 1)))
    glu_cot = conv_taps[0][:, None] * padded[:, :TOKENS]
    for lag in range(1, CONV_K):
        glu_cot = glu_cot + conv_taps[lag][:, None] * padded[:, lag:lag + TOKENS]
    gate_sigma = jax.nn.sigmoid(glu_gate.astype(jnp.float32))
    value_grad = (glu_cot * gate_sigma).astype(jnp.bfloat16)
    gate_in_grad = (glu_cot * glu_value.astype(jnp.float32) * gate_sigma * (1.0 - gate_sigma)).astype(jnp.bfloat16)
    return gate_grad, up_grad, down_grad, proj_grad, value_grad, gate_in_grad
```

```python
import jax
import jax.numpy as jnp
from jax import lax
from jax.sharding import PartitionSpec as P

D = 2048
C = 2048


def from_behind(value, axis, by):
    devices = lax.axis_size(axis)
    pairs = [(i, i + by) for i in range(devices) if 0 <= i + by < devices]
    return lax.ppermute(value, axis, pairs)


def contract(left, right, left_dim, right_dim):
    return lax.dot_general(
        left, right, (((left_dim,), (right_dim,)), ((), ())), preferred_element_type=jnp.float32
    )


def exchange(value, axis, by):
    devices = lax.axis_size(axis)
    return lax.ppermute(value, axis, [(i, i ^ by) for i in range(devices)])


def pick(value, index):
    return lax.dynamic_index_in_dim(value, index, 0, keepdims=False)


def fetch(mine):
    if lax.axis_size("sp") != 4:
        return [mine] + [exchange(mine, "sp", by) for by in range(1, lax.axis_size("sp"))]
    cut = mine.shape[0] // 2
    first, second = exchange(mine, "sp", 1), exchange(mine, "sp", 2)
    third = [exchange(first[:cut], "sp", 2), exchange(second[cut:], "sp", 1)]
    return [mine, first, second, jnp.concatenate(third, axis=0)]


def spread(pieces, rest):
    other = [rest] + [exchange(piece, "tp", 1) for piece in pieces[1:]]
    return jnp.concatenate(pieces + other, axis=0)


def halves(value, core):
    pair = value.reshape((2, value.shape[0] // 2) + value.shape[1:])
    return pick(pair, core), pick(pair, 1 - core)


def by_bits(value, index):
    count = value.shape[0]
    bit = 1
    while bit < count:
        order = [j ^ bit for j in range(count)]
        swapped = jnp.stack([value[j] for j in order])
        value = jnp.where((index & bit) != 0, swapped, value)
        bit *= 2
    return value


def on_device(
    saved_input,
    cotangent,
    expert_ids,
    route_weight,
    w_gate,
    w_up,
    w_down,
    w_out,
    channel_gain,
    conv_taps,
    glu_value,
    glu_gate,
    conv_out,
    norm_mean,
    norm_rstd,
):
    tokens_here = cotangent.shape[0]
    half = tokens_here // 2
    sp_count = lax.axis_size("sp")
    tp_count = lax.axis_size("tp")
    here = lax.axis_index("sp")
    place = lax.axis_index("tp")
    core, depth = place % 2, place // 2
    depths = tp_count // 2
    rows = sp_count * half
    wg, wu, wd = w_gate[0], w_up[0], w_down[0]

    mine_w, other_w = [], []
    for by in range(sp_count):
        weight = jnp.sum(jnp.where(expert_ids == (here ^ by), route_weight, 0.0), axis=1)
        if by:
            weight = exchange(weight, "sp", by)
        pair = weight.reshape(2, half)
        mine_w.append(pick(pair, core))
        other_w.append(pick(pair, 1 - core))
    weights = jnp.concatenate(mine_w + other_w, axis=0)

    few = sp_count == 4
    in_mine, in_other = halves(saved_input, core)
    in_mine, weights = lax.optimization_barrier((in_mine, weights))
    in_pieces = fetch(in_mine)
    rows_in = spread(in_pieces, in_other)
    cot_mine, cot_other = halves(cotangent, core)
    if few:
        cot_mine, _ = lax.optimization_barrier((cot_mine, in_pieces[1:3]))
    else:
        cot_mine, rows_in = lax.optimization_barrier((cot_mine, rows_in))
    cot_pieces = fetch(cot_mine)
    gate_pre = jnp.dot(rows_in, wg, preferred_element_type=jnp.float32)
    up_pre = jnp.dot(rows_in, wu, preferred_element_type=jnp.float32)
    cot_pieces, gate_pre, up_pre = lax.optimization_barrier((cot_pieces, gate_pre, up_pre))
    rows_cot = spread(cot_pieces, cot_other)
    rows_cot = (weights[:, None] * rows_cot.astype(jnp.float32)).astype(jnp.bfloat16)

    sigma = jax.nn.sigmoid(gate_pre)
    hidden = (gate_pre * sigma * up_pre).astype(jnp.bfloat16)
    hidden_cot = contract(rows_cot, wd, 1, 1)
    gate_cot = (hidden_cot * up_pre * sigma * (1.0 + gate_pre * (1.0 - sigma))).astype(jnp.bfloat16)
    up_cot = (hidden_cot * gate_pre * sigma).astype(jnp.bfloat16)

    gate_grad = contract(rows_in, gate_cot, 0, 0).astype(jnp.bfloat16)[None]
    up_grad = contract(rows_in, up_cot, 0, 0).astype(jnp.bfloat16)[None]
    down_grad = contract(hidden, rows_cot, 0, 0).astype(jnp.bfloat16)[None]
    if not few:
        gate_cot, up_cot, gate_grad, up_grad, down_grad = lax.optimization_barrier(
            (gate_cot, up_cot, gate_grad, up_grad, down_grad)
        )

    def input_part(first):
        return contract(gate_cot[first : first + rows], wg, 1, 1) + contract(
            up_cot[first : first + rows], wu, 1, 1
        )

    arrived = exchange(input_part(rows).astype(jnp.bfloat16), "tp", 1)
    if not few:
        arrived, gate_cot, up_cot = lax.optimization_barrier((arrived, gate_cot, up_cot))
    paired = (input_part(0) + arrived.astype(jnp.float32)).astype(jnp.bfloat16)
    blocks = paired.reshape(sp_count, half, D)
    if few:
        cut = half // 2
        wide = blocks.astype(jnp.float32)
        top = exchange(blocks[1::2, :cut], "sp", 1)
        low = exchange(blocks[2:, cut:], "sp", 2)
        top, low, down_grad = lax.optimization_barrier((top, low, down_grad))
        top, low = top.astype(jnp.float32), low.astype(jnp.float32)
        top_sent = exchange((wide[2, :cut] + top[1]).astype(jnp.bfloat16), "sp", 2)
        low_sent = exchange((wide[1, cut:] + low[1]).astype(jnp.bfloat16), "sp", 1)
        top_sent, low_sent, gate_grad, up_grad = lax.optimization_barrier(
            (top_sent, low_sent, gate_grad, up_grad)
        )
        total = jnp.concatenate(
            [
                wide[0, :cut] + top[0] + top_sent.astype(jnp.float32),
                wide[0, cut:] + low[0] + low_sent.astype(jnp.float32),
            ],
            axis=0,
        )
    else:
        total = blocks[0].astype(jnp.float32)
        for by in range(1, sp_count):
            total = total + exchange(blocks[by], "sp", by).astype(jnp.float32)
    shares = total.astype(jnp.bfloat16).reshape(depths, half // depths, D)
    total = pick(shares, depth).astype(jnp.float32)
    for by in range(1, depths):
        total = total + exchange(pick(shares, depth ^ by), "tp", 2 * by).astype(jnp.float32)
    total = total.astype(jnp.bfloat16)
    gathered = [total] + [exchange(total, "tp", 2 * by) for by in range(1, depths)]
    mine = by_bits(jnp.stack(gathered), depth).reshape(half, D)
    other = exchange(mine, "tp", 1)
    summed = by_bits(jnp.stack([mine, other]), core).reshape(tokens_here, D)
    mixed_cot = (cotangent.astype(jnp.float32) + summed.astype(jnp.float32)).astype(jnp.bfloat16)

    centered = (conv_out.astype(jnp.float32) - norm_mean[None, :]) * norm_rstd[None, :]
    normed = centered * channel_gain[:, None]
    sigma = jax.nn.sigmoid(normed)
    output_act = (normed * sigma).astype(jnp.bfloat16)
    proj_part = contract(mixed_cot, output_act, 0, 1).astype(jnp.bfloat16)
    mixed_cot, proj_part = lax.optimization_barrier((mixed_cot, proj_part))
    proj_part = proj_part.reshape(sp_count, D // sp_count, proj_part.shape[1])
    proj_grad = pick(proj_part, here).astype(jnp.float32)
    for by in range(1, sp_count):
        proj_grad = proj_grad + exchange(pick(proj_part, here ^ by), "sp", by).astype(jnp.float32)
    act_cot = contract(w_out, mixed_cot, 0, 1)
    norm_cot = act_cot * sigma * (1.0 + normed * (1.0 - sigma)) * channel_gain[:, None]
    sums = jnp.stack([jnp.sum(norm_cot, axis=0), jnp.sum(norm_cot * centered, axis=0)])
    first_sum, second_sum = sums + sum(exchange(sums, "tp", by) for by in range(1, tp_count))
    conv_cot = norm_rstd[None, :] * (
        norm_cot - first_sum[None, :] / C - centered * second_sum[None, :] / C
    )
    reach = conv_taps.shape[0] - 1
    rim = from_behind(conv_cot[:, :reach], "sp", -1)
    padded = jnp.concatenate([conv_cot, rim], axis=1)
    glu_cot = conv_taps[0][:, None] * padded[:, :tokens_here]
    for lag in range(1, reach + 1):
        glu_cot = glu_cot + conv_taps[lag][:, None] * padded[:, lag : lag + tokens_here]
    gate_sigma = jax.nn.sigmoid(glu_gate.astype(jnp.float32))
    value_grad = (glu_cot * gate_sigma).astype(jnp.bfloat16)
    gate_in_grad = (
        glu_cot * glu_value.astype(jnp.float32) * gate_sigma * (1.0 - gate_sigma)
    ).astype(jnp.bfloat16)
    return (gate_grad, up_grad, down_grad, proj_grad, value_grad, gate_in_grad)


def solution(mesh):
    in_specs = (
        P("sp", None),
        P("sp", None),
        P("sp", None),
        P("sp", None),
        P("sp", None, "tp"),
        P("sp", None, "tp"),
        P("sp", "tp", None),
        P(None, "tp"),
        P("tp"),
        P(None, "tp"),
        P("tp", "sp"),
        P("tp", "sp"),
        P("tp", "sp"),
        P("sp"),
        P("sp"),
    )
    out_specs = (
        P("sp", None, "tp"),
        P("sp", None, "tp"),
        P("sp", "tp", None),
        P("sp", "tp"),
        P("tp", "sp"),
        P("tp", "sp"),
    )
    return jax.shard_map(
        on_device, mesh=mesh, in_specs=in_specs, out_specs=out_specs, check_vma=False
    )
```
